32 devices in a mesh: sp: 8 (over z, x), tp: 4 (over y, core).
Axes of the slice: x: 2, y: 2, z: 4, core: 2. Of those that a mesh axis runs over, the one named last changes fastest.
Arguments:
- broad_probe_tensor: bfloat16 [4096, 1024], P('sp', 'tp'), may hold values from -6 to 6
- broad_lookup_tensor: bfloat16 [4096, 1024], P('sp', 'tp'), may hold values from -6 to 6
- broad_payload_tensor: bfloat16 [4096, 1024], P('sp', 'tp'), may hold values from -6 to 6
- broad_emission_valve: bfloat16 [4096, 1024], P('sp', 'tp'), may hold values from -6 to 6
- slim_probe_tensor: bfloat16 [4096, 1024], P('sp', 'tp'), may hold values from -6 to 6
- slim_lookup_tensor: bfloat16 [4096, 1024], P('sp', 'tp'), may hold values from -6 to 6
- slim_payload_tensor: bfloat16 [4096, 1024], P('sp', 'tp'), may hold values from -6 to 6
- slim_emission_valve: bfloat16 [4096, 1024], P('sp', 'tp'), may hold values from -6 to 6
- broad_forgetting_speed: float32 [8], P('tp'), may hold values from -0.08 to 0
- slim_forgetting_speed: float32 [16], P('tp'), may hold values from -0.08 to 0
- broad_channel_scaling: float32 [1024], P('tp'), may hold values from 0.1 to 1.9
- slim_channel_scaling: float32 [1024], P('tp'), may hold values from 0.1 to 1.9
- surge_forgetting: float32 [4096], P('sp'), may hold values from -2.1 to 0
- broad_emission_proj: bfloat16 [1024, 2048], replicated, may hold values from -0.125 to 0.125
- slim_emission_proj: bfloat16 [1024, 2048], replicated, may hold values from -0.125 to 0.125
- skip_stream: bfloat16 [4096, 2048], P(('sp', 'tp')), may hold values from -6 to 6
- premix_scaling_coeffs: float32 [2048], replicated, may hold values from 0.1 to 1.9
- routed_specialist_ids: int32 [4096, 2], P('sp'), may hold values from 0 to 7, as said below
- routed_specialist_shares: float32 [4096, 2], P('sp'), may hold values from 0.2 to 1
- specialist_valve_proj: bfloat16 [8, 2048, 2048], P('sp', None, 'tp'), may hold values from -0.125 to 0.125
- specialist_expand_proj: bfloat16 [8, 2048, 2048], P('sp', None, 'tp'), may hold values from -0.125 to 0.125
- specialist_contract_proj: bfloat16 [8, 2048, 2048], P('sp', 'tp'), may hold values from -0.125 to 0.125
Outputs:
- result: bfloat16 [4096, 2048], P(('sp', 'tp'))
The draws below stay inside these ranges and needn't reach their ends.
Inputs may be any that keep to these rules, and one draw needn't show every extreme that they name: `routed_specialist_ids`: each row names two different experts of one group, that is of the same run of 2 consecutive experts. The rows of one device (each aligned block of 128 rows) name each expert at most 64 times, and some expert is named exactly 64 times by the rows of every device.
All inputs are finite; a program needn't handle non-finite values.
Results may differ from the reference program's by a relative error of at most 0.018.
Values may be sent and summed in bfloat16 or wider, within the bound.
A program may use at most 128 MiB of HBM per device.

```python
import jax
import jax.numpy as jnp
from jax import lax

D = 2048
HA = 8
BROAD_CHANNEL_DIM = 128
HB = 16
THIN_CHANNEL_DIM = 64
FFE = 2048
GROUPS = 4
EXPERTS = 8
EXP_GROUP = 2
ROWS = 128
CAP = 64
TOKENS = 4096
BLOCK = 512
N_SP = 8
N_TP = 4


def rate_law(key, heads):
    pick_key, fast_key, slow_key = jax.random.split(key, 3)
    share = 5
    fast = jax.random.randint(pick_key, (heads,), 0, 10) < share
    span = jax.random.uniform(fast_key, (heads,), jnp.float32, 30.0, 100.0)
    slow = jnp.exp(jax.random.uniform(slow_key, (heads,), jnp.float32, jnp.log(0.02), jnp.log(0.2))) / TOKENS
    return jnp.where(fast, -jnp.log(10.0) / span, -slow).astype(jnp.float32)


def draw_broad_forgetting_speed(key, part):
    return rate_law(jax.random.fold_in(key, 11), HA)


def draw_slim_forgetting_speed(key, part):
    return rate_law(jax.random.fold_in(key, 12), HB)


def draw_surge_forgetting(key, part):
    where_key, size_key = jax.random.split(jax.random.fold_in(key, 21))
    spots = jax.random.randint(where_key, (3,), 0, TOKENS)
    kept = jax.random.uniform(size_key, (3,), jnp.float32, 0.5, 0.8)
    places = jnp.arange(TOKENS, dtype=jnp.int32)
    marks = jnp.where(places[None, :] == spots[:, None], jnp.log(kept)[:, None], 0.0)
    return jnp.sum(marks, 0).astype(jnp.float32)


def draw_routed_specialist_ids(key, part):
    base = jax.random.fold_in(key, 31)
    busy = jax.random.randint(jax.random.fold_in(base, 0), (), 0, GROUPS)
    blocks = TOKENS // ROWS
    units = CAP // 2

    def one(index):
        block_key = jax.random.fold_in(base, index + 1)
        cut_key, perm_key, offset_key, stride_key = jax.random.split(block_key, 4)
        cuts = jnp.sort(jax.random.randint(cut_key, (GROUPS - 2,), 0, units + 1))
        edges = jnp.concatenate([jnp.zeros((1,), jnp.int32), cuts, jnp.full((1,), units, jnp.int32)])
        counts = jnp.concatenate([jnp.full((1,), ROWS // 2, jnp.int32), (edges[1:] - edges[:-1]) * EXP_GROUP])
        ends = jnp.cumsum(counts)
        starts = ends - counts
        slot = jax.random.permutation(perm_key, ROWS)
        order = jnp.sum((slot[:, None] >= ends[None, :]).astype(jnp.int32), 1)
        inside = slot - starts[order]
        group = (busy + order) % GROUPS
        segment_begin = jax.random.randint(offset_key, (GROUPS,), 0, EXP_GROUP)
        stride = jax.random.randint(stride_key, (GROUPS,), 1, EXP_GROUP)
        first = group * EXP_GROUP + (segment_begin[group] + inside) % EXP_GROUP
        second = group * EXP_GROUP + (segment_begin[group] + inside + stride[group]) % EXP_GROUP
        return jnp.stack([first, second], 1)
    return jax.vmap(one)(jnp.arange(blocks, dtype=jnp.int32)).reshape(TOKENS, 2).astype(jnp.int32)


def steps_of(rng, dims, shards, smallest, largest):
    loudness = 1.0
    for position, parts in shards:
        heights = jax.random.uniform(jax.random.fold_in(jax.random.fold_in(rng, 6), position), (parts,), jnp.float32, smallest / len(shards), largest / len(shards))
        loudness = loudness * jnp.repeat(jnp.exp(heights), dims[position] // parts).reshape((-1,) + (1,) * (len(dims) - 1 - position))
    return loudness


def noise(stream_key, dims, scale, limit, cuts=(), kind=jnp.bfloat16):
    loudness = steps_of(stream_key, dims, cuts, -0.22, 0.18) if cuts else 1.0
    entries = jax.random.normal(stream_key, dims, jnp.float32) * scale * loudness
    return jnp.minimum(jnp.maximum(entries, -limit), limit).astype(kind)


def setup_inputs(seed: int = 0) -> dict:
    keys = jax.random.split(jax.random.key(seed), 23)
    return {
        "broad_probe_tensor": noise(keys[0], (TOKENS, HA * BROAD_CHANNEL_DIM), 1.0, 6.0, ((0, 8), (1, 4))),
        "broad_lookup_tensor": noise(keys[1], (TOKENS, HA * BROAD_CHANNEL_DIM), 1.0, 6.0, ((0, 8), (1, 4))),
        "broad_payload_tensor": noise(keys[2], (TOKENS, HA * BROAD_CHANNEL_DIM), 1.0, 6.0, ((0, 8), (1, 4))),
        "broad_emission_valve": noise(keys[3], (TOKENS, HA * BROAD_CHANNEL_DIM), 1.0, 6.0, ((0, 8), (1, 4))),
        "slim_probe_tensor": noise(keys[4], (TOKENS, HB * THIN_CHANNEL_DIM), 1.0, 6.0, ((0, 8), (1, 4))),
        "slim_lookup_tensor": noise(keys[5], (TOKENS, HB * THIN_CHANNEL_DIM), 1.0, 6.0, ((0, 8), (1, 4))),
        "slim_payload_tensor": noise(keys[6], (TOKENS, HB * THIN_CHANNEL_DIM), 1.0, 6.0, ((0, 8), (1, 4))),
        "slim_emission_valve": noise(keys[7], (TOKENS, HB * THIN_CHANNEL_DIM), 1.0, 6.0, ((0, 8), (1, 4))),
        "broad_forgetting_speed": draw_broad_forgetting_speed(jax.random.fold_in(keys[22], 71), 0),
        "slim_forgetting_speed": draw_slim_forgetting_speed(jax.random.fold_in(keys[22], 71), 0),
        "broad_channel_scaling": jnp.clip(1.0 + 0.18 * jax.random.normal(keys[10], (HA * BROAD_CHANNEL_DIM,), jnp.float32), 0.1, 1.9),
        "slim_channel_scaling": jnp.clip(1.0 + 0.18 * jax.random.normal(keys[11], (HB * THIN_CHANNEL_DIM,), jnp.float32), 0.1, 1.9),
        "surge_forgetting": draw_surge_forgetting(jax.random.fold_in(keys[22], 71), 0),
        "broad_emission_proj": noise(keys[13], (HA * BROAD_CHANNEL_DIM, D), (HA * BROAD_CHANNEL_DIM + HB * THIN_CHANNEL_DIM) ** -0.5, 0.125),
        "slim_emission_proj": noise(keys[14], (HB * THIN_CHANNEL_DIM, D), (HA * BROAD_CHANNEL_DIM + HB * THIN_CHANNEL_DIM) ** -0.5, 0.125),
        "skip_stream": noise(keys[15], (TOKENS, D), 1.0, 6.0, ((0, 32),)),
        "premix_scaling_coeffs": jnp.clip(1.0 + 0.18 * jax.random.normal(keys[16], (D,), jnp.float32), 0.1, 1.9),
        "routed_specialist_ids": draw_routed_specialist_ids(jax.random.fold_in(keys[22], 71), 0),
        "routed_specialist_shares": jnp.clip(0.2 + 0.8 * jax.random.uniform(keys[18], (TOKENS, 2), jnp.float32) ** steps_of(keys[18], (TOKENS, 2), ((0, 8),), -0.2, 0.2), 0.2, 1.0),
        "specialist_valve_proj": noise(keys[19], (EXPERTS, D, FFE), D ** -0.5, 0.125, ((0, 8), (2, 4))),
        "specialist_expand_proj": noise(keys[20], (EXPERTS, D, FFE), D ** -0.5, 0.125, ((0, 8), (2, 4))),
        "specialist_contract_proj": noise(keys[21], (EXPERTS, FFE, D), FFE ** -0.5, 0.125, ((0, 8), (1, 4))),
    }


rope_base = 10000.0
epsilon = 1e-06

def rotate(payload_tensor, positions):
    channel_dimension = payload_tensor.shape[-1]
    half = channel_dimension // 2
    freq = rope_base ** (-jnp.arange(half, dtype=jnp.float32) * 2.0 / channel_dimension)
    angle = positions.astype(jnp.float32)[:, None, None] * freq[None, None, :]
    cosine = jnp.cos(angle)
    sine = jnp.sin(angle)
    first = payload_tensor[..., :half]
    second = payload_tensor[..., half:]
    return jnp.concatenate([first * cosine - second * sine, first * sine + second * cosine], -1)

def prepare(probe_source, lookup_tensor, payload_tensor, heads, channel_dimension):
    length = probe_source.shape[0]
    places = jnp.arange(length, dtype=jnp.int32)
    spun_probe = rotate(probe_source.astype(jnp.float32).reshape(length, heads, channel_dimension), places).astype(jnp.bfloat16)
    spun_lookup = (rotate(lookup_tensor.astype(jnp.float32).reshape(length, heads, channel_dimension), places) * channel_dimension ** (-0.5)).astype(jnp.bfloat16)
    return (spun_probe, spun_lookup, payload_tensor.reshape(length, heads, channel_dimension))

def segment_terms(probe_tensor, lookup_tensor, payload_tensor, surge_forgetting, forgetting_speed):
    length = probe_tensor.shape[0]
    segment_tally = jnp.arange(length, dtype=jnp.float32)
    memory_matrix = forgetting_speed[None, :] * segment_tally[:, None] + jnp.cumsum(surge_forgetting)[:, None]
    causal = (segment_tally[:, None] >= segment_tally[None, :])[None]
    level_t = jnp.transpose(memory_matrix)
    gap = level_t[:, :, None] - level_t[:, None, :]
    decay = jnp.where(causal, jnp.exp(jnp.where(causal, gap, 0.0)), 0.0)
    attention_scores = jnp.einsum('szr,yzr->zsy', probe_tensor.astype(jnp.float32), lookup_tensor.astype(jnp.float32))
    weights = (attention_scores * decay).astype(jnp.bfloat16)
    inner = jnp.einsum('htm,mhe->the', weights.astype(jnp.float32), payload_tensor.astype(jnp.float32))
    factor = jnp.exp(memory_matrix + forgetting_speed[None, :])
    tail = jnp.exp(memory_matrix[-1:, :] - memory_matrix)
    weighted_output = (lookup_tensor.astype(jnp.float32) * tail[:, :, None]).astype(jnp.bfloat16)
    state_update = jnp.einsum('oup,our->upr', weighted_output.astype(jnp.float32), payload_tensor.astype(jnp.float32))
    total = jnp.exp(memory_matrix[-1] + forgetting_speed)
    return (inner, factor, state_update, total)

def read_state(probe_tensor, state):
    return jnp.einsum('thd,hde->the', probe_tensor.astype(jnp.float32), state, precision=lax.Precision.HIGHEST)

def finish(sublayer_final, emission_valve, scaling_coefficients):
    length, heads, channel_dimension = sublayer_final.shape
    normed = sublayer_final * lax.rsqrt(lax.optimization_barrier(jnp.mean(sublayer_final * sublayer_final, -1, keepdims=True)) + epsilon)
    gated = normed.reshape(length, heads * channel_dimension) * scaling_coefficients[None, :] * jax.nn.silu(emission_valve.astype(jnp.float32))
    return gated.astype(jnp.bfloat16)

def keeping_multiplier(probe_source, lookup_tensor, payload_tensor, emission_valve, forgetting_speed, scaling_coefficients, surge_forgetting, channel_dimension):
    heads = probe_source.shape[1] // channel_dimension
    spun_probe, spun_lookup, regrouped_payload = prepare(probe_source, lookup_tensor, payload_tensor, heads, channel_dimension)
    count = TOKENS // BLOCK

    def divider_mark(array):
        return array.reshape((count, BLOCK) + array.shape[1:])

    def segment_walker(state, piece):
        block_q, block_k, block_v, block_b = piece
        inner, factor, state_update, total = segment_terms(block_q, block_k, block_v, block_b, forgetting_speed)
        sublayer_final = inner + factor[:, :, None] * read_state(block_q, state)
        return (total[:, None, None] * state + state_update, sublayer_final)
    opening_location = jnp.zeros((heads, channel_dimension, channel_dimension), jnp.float32)
    ignored_placeholder, sublayer_final = lax.scan(segment_walker, opening_location, (divider_mark(spun_probe), divider_mark(spun_lookup), divider_mark(regrouped_payload), divider_mark(surge_forgetting)))
    return finish(sublayer_final.reshape(TOKENS, heads, channel_dimension), emission_valve, scaling_coefficients)

def experts_mix(normed, routed_specialist_ids, routed_specialist_shares, specialist_valve_proj, specialist_expand_proj, specialist_contract_proj):
    most = N_SP * N_TP * CAP
    slice_width = FFE // N_TP
    padded = jnp.concatenate([normed, jnp.zeros((1, D), jnp.bfloat16)], 0)

    def one(accum, index):
        matches = routed_specialist_ids == index
        weight = lax.optimization_barrier(jnp.sum(jnp.where(matches, routed_specialist_shares, 0.0), 1))
        weight = jnp.concatenate([weight, jnp.zeros((1,), jnp.float32)], 0)
        picked = jnp.nonzero(jnp.any(matches, 1), size=most, fill_value=TOKENS)[0].astype(jnp.int32)
        taken = padded[picked]
        emission_valve = jnp.dot(taken, specialist_valve_proj[index], preferred_element_type=jnp.float32)
        up = jnp.dot(taken, specialist_expand_proj[index], preferred_element_type=jnp.float32)
        hidden = (jax.nn.silu(emission_valve) * up).astype(jnp.bfloat16).reshape(most, N_TP, slice_width)
        down = specialist_contract_proj[index].reshape(N_TP, slice_width, D)
        partial_value = jnp.einsum('mpf,pfd->pmd', hidden.astype(jnp.float32), down.astype(jnp.float32))
        rounded = lax.optimization_barrier(partial_value.astype(jnp.bfloat16))
        expert_out = lax.optimization_barrier(jnp.sum(rounded.astype(jnp.float32), 0)).astype(jnp.bfloat16)
        accum = accum.at[picked].add(weight[picked][:, None] * expert_out.astype(jnp.float32))
        return (accum, None)
    opening_location = jnp.zeros((TOKENS + 1, D), jnp.float32)
    accum, ignored_placeholder = lax.scan(one, opening_location, jnp.arange(EXPERTS, dtype=jnp.int32))
    return accum[:TOKENS]

def reference(broad_probe_tensor, broad_lookup_tensor, broad_payload_tensor, broad_emission_valve, slim_probe_tensor, slim_lookup_tensor, slim_payload_tensor, slim_emission_valve, broad_forgetting_speed, slim_forgetting_speed, broad_channel_scaling, slim_channel_scaling, surge_forgetting, broad_emission_proj, slim_emission_proj, skip_stream, premix_scaling_coeffs, routed_specialist_ids, routed_specialist_shares, specialist_valve_proj, specialist_expand_proj, specialist_contract_proj):
    broad_channel_total = keeping_multiplier(broad_probe_tensor, broad_lookup_tensor, broad_payload_tensor, broad_emission_valve, broad_forgetting_speed, broad_channel_scaling, surge_forgetting, BROAD_CHANNEL_DIM)
    slim_channel_total = keeping_multiplier(slim_probe_tensor, slim_lookup_tensor, slim_payload_tensor, slim_emission_valve, slim_forgetting_speed, slim_channel_scaling, surge_forgetting, THIN_CHANNEL_DIM)
    projected = jnp.dot(broad_channel_total, broad_emission_proj, preferred_element_type=jnp.float32)
    projected = projected + jnp.dot(slim_channel_total, slim_emission_proj, preferred_element_type=jnp.float32)
    updated = skip_stream.astype(jnp.float32) + projected
    scale = lax.rsqrt(lax.optimization_barrier(jnp.mean(updated * updated, -1, keepdims=True)) + epsilon)
    normed = (updated * scale * premix_scaling_coeffs[None, :]).astype(jnp.bfloat16)
    mixture = experts_mix(normed, routed_specialist_ids, routed_specialist_shares, specialist_valve_proj, specialist_expand_proj, specialist_contract_proj)
    return (updated + mixture).astype(jnp.bfloat16)
```

```python
import jax
import jax.numpy as jnp
from jax import lax
from jax.experimental import pallas as pl
from jax.experimental.pallas import tpu as pltpu
from jax.sharding import PartitionSpec as P

MESH = pl.DeviceIdType.MESH
VMEM_SPEC = pl.BlockSpec(memory_space=pltpu.VMEM)

BROAD_CHANNEL_DIM = 128
THIN_CHANNEL_DIM = 64
GROUPS = 4


rope_base = 10000.0
epsilon = 1e-06


def exchange_kernel(state_ref, tile_ref, states_ref, tiles_ref, send_sem, recv_sem):
    me = lax.axis_index("sp")
    count = states_ref.shape[0]
    barrier = pltpu.get_barrier_semaphore()
    for step in range(1, count):
        pl.semaphore_signal(
            barrier, inc=1, device_id={"sp": lax.rem(me + step, count)}, device_id_type=MESH
        )
    pl.semaphore_wait(barrier, count - 1)
    copies = []
    for step in range(1, count):
        for kind, (src, dst) in enumerate(((state_ref, states_ref), (tile_ref, tiles_ref))):
            copy = pltpu.make_async_remote_copy(
                src_ref=src,
                dst_ref=dst.at[me],
                send_sem=send_sem.at[kind, step],
                recv_sem=recv_sem.at[kind, step],
                device_id={"sp": lax.rem(me + step, count)},
                device_id_type=MESH,
            )
            copy.start()
            copies.append(copy)
    states_ref[me] = state_ref[...]
    tiles_ref[me] = tile_ref[...]
    for copy in copies:
        copy.wait()


def exchange(state, tile):
    count = lax.axis_size("sp")
    return pl.pallas_call(
        exchange_kernel,
        out_shape=(
            jax.ShapeDtypeStruct((count,) + state.shape, state.dtype),
            jax.ShapeDtypeStruct((count,) + tile.shape, tile.dtype),
        ),
        in_specs=[VMEM_SPEC] * 2,
        out_specs=(VMEM_SPEC, VMEM_SPEC),
        scratch_shapes=[
            pltpu.SemaphoreType.DMA((2, count)),
            pltpu.SemaphoreType.DMA((2, count)),
        ],
        compiler_params=pltpu.CompilerParams(collective_id=0, has_side_effects=True),
        name="state_exchange",
    )(state, tile)


def greet_group(groups, pair):
    me = lax.axis_index("sp")
    group = me // pair
    member = lax.rem(me, pair)
    barrier = pltpu.get_barrier_semaphore()
    for step in range(1, groups):
        pl.semaphore_signal(
            barrier,
            inc=1,
            device_id={"sp": lax.rem(group + step, groups) * pair + member},
            device_id_type=MESH,
        )
    pl.semaphore_signal(
        barrier, inc=1, device_id={"sp": group * pair + 1 - member}, device_id_type=MESH
    )
    pl.semaphore_wait(barrier, groups)
    return group, member


def dispatch_kernel(rows_ref, out_ref, send_far, recv_far, send_near, recv_near):
    groups = rows_ref.shape[0]
    pair = out_ref.shape[0]
    group, member = greet_group(groups, pair)
    partner = group * pair + 1 - member
    far = []
    for step in range(1, groups):
        target = lax.rem(group + step, groups)
        copy = pltpu.make_async_remote_copy(
            src_ref=rows_ref.at[target],
            dst_ref=out_ref.at[member, group],
            send_sem=send_far.at[step],
            recv_sem=recv_far.at[step],
            device_id={"sp": target * pair + member},
            device_id_type=MESH,
        )
        copy.start()
        far.append(copy)
    near = []
    for step in range(groups):
        origin = lax.rem(group - step + groups, groups)
        if step > 0:
            far[step - 1].wait_recv()
        copy = pltpu.make_async_remote_copy(
            src_ref=rows_ref.at[group] if step == 0 else out_ref.at[member, origin],
            dst_ref=out_ref.at[member, origin],
            send_sem=send_near.at[step],
            recv_sem=recv_near.at[step],
            device_id={"sp": partner},
            device_id_type=MESH,
        )
        copy.start()
        near.append(copy)
        if step == 0:
            out_ref[member, group] = rows_ref[group]
    for copy in far:
        copy.wait_send()
    for copy in near:
        copy.wait()


def dispatch(rows, pair):
    groups = rows.shape[0]
    return pl.pallas_call(
        dispatch_kernel,
        out_shape=jax.ShapeDtypeStruct((pair,) + rows.shape, rows.dtype),
        in_specs=[VMEM_SPEC],
        out_specs=VMEM_SPEC,
        scratch_shapes=[pltpu.SemaphoreType.DMA((groups,))] * 4,
        compiler_params=pltpu.CompilerParams(collective_id=1, has_side_effects=True),
        name="row_dispatch",
    )(rows)


def collect_kernel(parts_ref, out_ref, landed, joined, send_near, recv_near, send_far, recv_far):
    pair, groups = parts_ref.shape[:2]
    group, member = greet_group(groups, pair)
    partner = group * pair + 1 - member
    order = list(range(1, groups)) + [0]
    near = {}
    for step in order:
        target = lax.rem(group + step, groups)
        near[step] = pltpu.make_async_remote_copy(
            src_ref=parts_ref.at[1 - member, target],
            dst_ref=landed.at[target],
            send_sem=send_near.at[step],
            recv_sem=recv_near.at[step],
            device_id={"sp": partner},
            device_id_type=MESH,
        )
        near[step].start()
    far = []
    for step in order:
        target = lax.rem(group + step, groups)
        near[step].wait_recv()
        total = (
            parts_ref[member, target].astype(jnp.float32) + landed[target].astype(jnp.float32)
        ).astype(out_ref.dtype)
        if step == 0:
            out_ref[group] = total
        else:
            joined[target] = total
            copy = pltpu.make_async_remote_copy(
                src_ref=joined.at[target],
                dst_ref=out_ref.at[group],
                send_sem=send_far.at[step],
                recv_sem=recv_far.at[step],
                device_id={"sp": target * pair + member},
                device_id_type=MESH,
            )
            copy.start()
            far.append(copy)
    for step in order:
        near[step].wait_send()
    for copy in far:
        copy.wait()


def collect(parts):
    pair, groups = parts.shape[:2]
    return pl.pallas_call(
        collect_kernel,
        out_shape=jax.ShapeDtypeStruct(parts.shape[1:], parts.dtype),
        in_specs=[VMEM_SPEC],
        out_specs=VMEM_SPEC,
        scratch_shapes=[pltpu.VMEM(parts.shape[1:], parts.dtype)] * 2
        + [pltpu.SemaphoreType.DMA((groups,))] * 4,
        compiler_params=pltpu.CompilerParams(collective_id=2, has_side_effects=True),
        name="row_collect",
    )(parts)


def rotate(payload_tensor, positions):
    channel_dimension = payload_tensor.shape[-1]
    half = channel_dimension // 2
    freq = rope_base ** (-jnp.arange(half, dtype=jnp.float32) * 2.0 / channel_dimension)
    angle = positions.astype(jnp.float32)[:, None, None] * freq[None, None, :]
    cosine = jnp.cos(angle)
    sine = jnp.sin(angle)
    first = payload_tensor[..., :half]
    second = payload_tensor[..., half:]
    return jnp.concatenate([first * cosine - second * sine, first * sine + second * cosine], -1)


def segment_terms(probe_tensor, lookup_tensor, payload_tensor, surge_forgetting, forgetting_speed):
    length = probe_tensor.shape[0]
    segment_tally = jnp.arange(length, dtype=jnp.float32)
    memory_matrix = (
        forgetting_speed[None, :] * segment_tally[:, None] + jnp.cumsum(surge_forgetting)[:, None]
    )
    causal = (segment_tally[:, None] >= segment_tally[None, :])[None]
    level_t = jnp.transpose(memory_matrix)
    gap = level_t[:, :, None] - level_t[:, None, :]
    decay = jnp.where(causal, jnp.exp(jnp.where(causal, gap, 0.0)), 0.0)
    attention_scores = jnp.einsum(
        "szr,yzr->zsy", probe_tensor, lookup_tensor, preferred_element_type=jnp.float32
    )
    weights = (attention_scores * decay).astype(jnp.bfloat16)
    inner = jnp.einsum("htm,mhe->the", weights, payload_tensor, preferred_element_type=jnp.float32)
    factor = jnp.exp(memory_matrix + forgetting_speed[None, :])
    tail = jnp.exp(memory_matrix[-1:, :] - memory_matrix)
    weighted_output = (lookup_tensor.astype(jnp.float32) * tail[:, :, None]).astype(jnp.bfloat16)
    state_update = jnp.einsum(
        "oup,our->upr", weighted_output, payload_tensor, preferred_element_type=jnp.float32
    )
    total = memory_matrix[-1] + forgetting_speed
    return (inner, factor, state_update, total)


def read_state(probe_tensor, state):
    return jnp.einsum(
        "thd,hde->the", probe_tensor.astype(jnp.float32), state, precision=lax.Precision.HIGHEST
    )


def keeping_multiplier(
    probe_source,
    lookup_tensor,
    payload_tensor,
    forgetting_speed,
    surge_forgetting,
    channel_dimension,
    segment_begin,
):
    length = probe_source.shape[0]
    heads = probe_source.shape[1] // channel_dimension
    places = segment_begin + jnp.arange(length, dtype=jnp.int32)
    spun_probe = rotate(
        probe_source.astype(jnp.float32).reshape(length, heads, channel_dimension), places
    ).astype(jnp.bfloat16)
    spun_lookup = (
        rotate(lookup_tensor.astype(jnp.float32).reshape(length, heads, channel_dimension), places)
        * channel_dimension ** (-0.5)
    ).astype(jnp.bfloat16)
    regrouped_payload = payload_tensor.reshape(length, heads, channel_dimension)
    block = min(512, length)
    count = length // block

    def divider_mark(array):
        return array.reshape((count, block) + array.shape[1:])

    state, level, local, reach = None, None, [], []
    for piece in zip(
        divider_mark(spun_probe),
        divider_mark(spun_lookup),
        divider_mark(regrouped_payload),
        divider_mark(surge_forgetting),
    ):
        inner, factor, state_update, total = segment_terms(*piece, forgetting_speed)
        if state is None:
            state, level = state_update, total
        else:
            inner = inner + factor[:, :, None] * read_state(piece[0], state)
            factor = factor * jnp.exp(level)[None, :]
            state, level = jnp.exp(total)[:, None, None] * state + state_update, level + total
        local.append(inner)
        reach.append(factor)
    return (
        spun_probe,
        jnp.concatenate(local, 0),
        jnp.concatenate(reach, 0),
        level,
        state,
    )


def finish(sublayer_final, emission_valve, scaling_coefficients):
    length, heads, channel_dimension = sublayer_final.shape
    normed = sublayer_final * lax.rsqrt(
        jnp.mean(sublayer_final * sublayer_final, -1, keepdims=True) + epsilon
    )
    gated = (
        normed.reshape(length, heads * channel_dimension)
        * scaling_coefficients[None, :]
        * jax.nn.silu(emission_valve.astype(jnp.float32))
    )
    return gated.astype(jnp.bfloat16)


def carried(states, levels):
    place = lax.axis_index("sp")
    count = states.shape[0]
    index = jnp.arange(count, dtype=jnp.int32)
    between = (index[None, :] > index[:, None]) & (index[None, :] < place)
    reach = jnp.sum(jnp.where(between[:, :, None], levels[None, :, :], 0.0), 1)
    weight = jnp.where((index < place)[:, None], jnp.exp(reach), 0.0)
    return jnp.sum(weight[:, :, None, None] * states.astype(jnp.float32), 0)


def slot_positions(chosen, experts, cap):
    listed = chosen.reshape(-1)
    matches = (listed[:, None] == jnp.arange(experts, dtype=jnp.int32)[None, :]).astype(jnp.int32)
    before = jnp.cumsum(matches, 0) - matches
    order = jnp.sum(before * matches, 1)
    return (listed * cap + order).reshape(chosen.shape)


def fill_slots(rows_in, chosen, experts, cap):
    count = rows_in.shape[0]
    places = slot_positions(chosen, experts, cap).reshape(-1)
    owners = jnp.repeat(jnp.arange(count, dtype=jnp.int32), 2)
    source = jnp.full((experts * cap,), count, jnp.int32).at[places].set(owners)
    padded = jnp.concatenate([rows_in, jnp.zeros((1, rows_in.shape[1]), rows_in.dtype)], 0)
    return padded[source].reshape(experts, cap, rows_in.shape[1])


def on_device(
    broad_probe_tensor,
    broad_lookup_tensor,
    broad_payload_tensor,
    broad_emission_valve,
    slim_probe_tensor,
    slim_lookup_tensor,
    slim_payload_tensor,
    slim_emission_valve,
    broad_forgetting_speed,
    slim_forgetting_speed,
    broad_channel_scaling,
    slim_channel_scaling,
    surge_forgetting,
    broad_emission_proj,
    slim_emission_proj,
    skip_stream,
    premix_scaling_coeffs,
    routed_specialist_ids,
    routed_specialist_shares,
    specialist_valve_proj,
    specialist_expand_proj,
    specialist_contract_proj,
):
    length = broad_probe_tensor.shape[0]
    segment_begin = lax.axis_index("sp") * length
    valve_all = lax.all_gather(specialist_valve_proj[0], "tp")
    expand_all = lax.all_gather(specialist_expand_proj[0], "tp")
    contract_all = lax.all_gather(specialist_contract_proj[0], "tp")
    wide_result = keeping_multiplier(
        broad_probe_tensor,
        broad_lookup_tensor,
        broad_payload_tensor,
        broad_forgetting_speed,
        surge_forgetting,
        BROAD_CHANNEL_DIM,
        segment_begin,
    )
    narrow_result = keeping_multiplier(
        slim_probe_tensor,
        slim_lookup_tensor,
        slim_payload_tensor,
        slim_forgetting_speed,
        surge_forgetting,
        THIN_CHANNEL_DIM,
        segment_begin,
    )
    rows = skip_stream.shape[0]
    width = skip_stream.shape[1]
    experts = lax.axis_size("sp") * specialist_valve_proj.shape[0]
    cap = rows * GROUPS // experts
    pair = experts // GROUPS
    own_ids = lax.dynamic_slice_in_dim(routed_specialist_ids, lax.axis_index("tp") * rows, rows, 0)
    own_weights = lax.dynamic_slice_in_dim(
        routed_specialist_shares, lax.axis_index("tp") * rows, rows, 0
    )
    levels = jnp.concatenate([wide_result[3], narrow_result[3]])
    tile = levels
    if pair == 2:
        group_of = own_ids[:, 0] // pair
        named = group_of[:, None] == jnp.arange(GROUPS, dtype=jnp.int32)[None, :]
        rank = jnp.cumsum(named.astype(jnp.int32), 0) - 1
        own_slot = group_of * cap + jnp.sum(jnp.where(named, rank, 0), 1)
        holds = own_slot[None, :] == jnp.arange(GROUPS * cap, dtype=jnp.int32)[:, None]
        member_ids = own_ids - group_of[:, None] * pair
        slot_shares = []
        for member in range(pair):
            share = jnp.sum(jnp.where(member_ids == member, own_weights, 0.0), 1)
            slot_shares.append(jnp.sum(jnp.where(holds, share[None, :], 0.0), 1))
        tile = jnp.concatenate([levels] + slot_shares)
    tile_size = -(-tile.shape[0] // 1024) * 1024
    tile = jnp.pad(tile, (0, tile_size - tile.shape[0])).reshape(-1, 128)
    packed = jnp.concatenate(
        [wide_result[4].reshape(-1, 128), narrow_result[4].reshape(-1, 128)], 0
    ).astype(jnp.bfloat16)
    states, tiles = exchange(packed, tile)
    count = states.shape[0]
    tiles = tiles.reshape(count, -1)
    wide_heads = wide_result[3].shape[0]
    both_heads = levels.shape[0]
    cut = wide_result[4].size // 128
    incoming_wide = carried(
        states[:, :cut].reshape((count,) + wide_result[4].shape), tiles[:, :wide_heads]
    )
    incoming_narrow = carried(
        states[:, cut:].reshape((count,) + narrow_result[4].shape),
        tiles[:, wide_heads:both_heads],
    )
    mixed_wide = finish(
        wide_result[1] + wide_result[2][:, :, None] * read_state(wide_result[0], incoming_wide),
        broad_emission_valve,
        broad_channel_scaling,
    )
    mixed_narrow = finish(
        narrow_result[1] + narrow_result[2][:, :, None] * read_state(narrow_result[0], incoming_narrow),
        slim_emission_valve,
        slim_channel_scaling,
    )
    rows_wide, rows_narrow = (
        lax.all_to_all(mixed_wide, "tp", split_axis=0, concat_axis=1, tiled=True),
        lax.all_to_all(mixed_narrow, "tp", split_axis=0, concat_axis=1, tiled=True),
    )
    projected = jnp.dot(rows_wide, broad_emission_proj, preferred_element_type=jnp.float32)
    projected = projected + jnp.dot(
        rows_narrow, slim_emission_proj, preferred_element_type=jnp.float32
    )
    updated = skip_stream.astype(jnp.float32) + projected
    scale = lax.rsqrt(jnp.mean(updated * updated, -1, keepdims=True) + epsilon)
    normed = (updated * scale * premix_scaling_coeffs[None, :]).astype(jnp.bfloat16)
    if pair == 2:
        spread = holds.astype(jnp.bfloat16)
        filled = jnp.dot(spread, normed, preferred_element_type=jnp.float32).astype(jnp.bfloat16)
        slots = dispatch(filled.reshape(GROUPS, cap, width), pair).reshape(-1, width)
    else:
        own_places = slot_positions(own_ids, experts, cap)
        slots = lax.all_to_all(
            fill_slots(normed, own_ids, experts, cap), "sp", split_axis=0, concat_axis=0, tiled=True
        ).reshape(-1, width)
    expert_out = None
    for part in range(lax.axis_size("tp")):
        emission_valve = jnp.dot(slots, valve_all[part], preferred_element_type=jnp.float32)
        up = jnp.dot(slots, expand_all[part], preferred_element_type=jnp.float32)
        hidden = (jax.nn.silu(emission_valve) * up).astype(jnp.bfloat16)
        term = jnp.dot(hidden, contract_all[part], preferred_element_type=jnp.float32)
        expert_out = term if expert_out is None else expert_out + term
    if pair == 2:
        place = lax.axis_index("sp")
        shares = tiles[:, both_heads : both_heads + pair * GROUPS * cap]
        shares = shares.reshape(GROUPS, pair, pair, GROUPS, cap)
        shares = lax.dynamic_index_in_dim(shares, place % pair, 2, False)
        shares = lax.dynamic_index_in_dim(shares, place // pair, 2, False)
        shares = jnp.transpose(shares, (1, 0, 2)).reshape(-1, 1)
        parts = (expert_out * shares).astype(jnp.bfloat16)
        returned = collect(parts.reshape(pair, GROUPS, cap, width)).reshape(-1, width)
        mixture = lax.dot_general(
            spread, returned, (((0,), (0,)), ((), ())), preferred_element_type=jnp.float32
        )
    else:
        returned = lax.all_to_all(
            expert_out.astype(jnp.bfloat16).reshape(experts, cap, width),
            "sp",
            split_axis=0,
            concat_axis=0,
            tiled=True,
        )
        picked = returned.reshape(experts * cap, width)[own_places]
        mixture = jnp.sum(own_weights[:, :, None] * picked.astype(jnp.float32), 1)
    return (updated + mixture).astype(jnp.bfloat16)


def solution(mesh):
    return jax.shard_map(
        on_device,
        mesh=mesh,
        in_specs=(
            P("sp", "tp"),
            P("sp", "tp"),
            P("sp", "tp"),
            P("sp", "tp"),
            P("sp", "tp"),
            P("sp", "tp"),
            P("sp", "tp"),
            P("sp", "tp"),
            P("tp"),
            P("tp"),
            P("tp"),
            P("tp"),
            P("sp"),
            P(),
            P(),
            P(("sp", "tp"), None),
            P(),
            P("sp", None),
            P("sp", None),
            P("sp", None, "tp"),
            P("sp", None, "tp"),
            P("sp", "tp", None),
        ),
        out_specs=P(("sp", "tp"), None),
        check_vma=False,
    )
```

```python
import jax
import jax.numpy as jnp
from jax import lax
from jax.experimental import pallas as pl
from jax.experimental.pallas import tpu as pltpu
from jax.sharding import PartitionSpec as P

MESH = pl.DeviceIdType.MESH
VMEM_SPEC = pl.BlockSpec(memory_space=pltpu.VMEM)

BROAD_CHANNEL_DIM = 128
THIN_CHANNEL_DIM = 64
GROUPS = 4


rope_base = 10000.0
epsilon = 1e-06


def exchange_kernel(state_ref, tile_ref, states_ref, tiles_ref, send_sem, recv_sem):
    me = lax.axis_index("sp")
    count = states_ref.shape[0]
    barrier = pltpu.get_barrier_semaphore()
    for step in range(1, count):
        pl.semaphore_signal(
            barrier, inc=1, device_id={"sp": lax.rem(me + step, count)}, device_id_type=MESH
        )
    pl.semaphore_wait(barrier, count - 1)
    copies = []
    for step in range(1, count):
        for kind, (src, dst) in enumerate(((state_ref, states_ref), (tile_ref, tiles_ref))):
            copy = pltpu.make_async_remote_copy(
                src_ref=src,
                dst_ref=dst.at[me],
                send_sem=send_sem.at[kind, step],
                recv_sem=recv_sem.at[kind, step],
                device_id={"sp": lax.rem(me + step, count)},
                device_id_type=MESH,
            )
            copy.start()
            copies.append(copy)
    states_ref[me] = state_ref[...]
    tiles_ref[me] = tile_ref[...]
    for copy in copies:
        copy.wait()


def exchange(state, tile):
    count = lax.axis_size("sp")
    return pl.pallas_call(
        exchange_kernel,
        out_shape=(
            jax.ShapeDtypeStruct((count,) + state.shape, state.dtype),
            jax.ShapeDtypeStruct((count,) + tile.shape, tile.dtype),
        ),
        in_specs=[VMEM_SPEC] * 2,
        out_specs=(VMEM_SPEC, VMEM_SPEC),
        scratch_shapes=[
            pltpu.SemaphoreType.DMA((2, count)),
            pltpu.SemaphoreType.DMA((2, count)),
        ],
        compiler_params=pltpu.CompilerParams(collective_id=0, has_side_effects=True),
        name="state_exchange",
    )(state, tile)


def greet_group(groups, pair):
    me = lax.axis_index("sp")
    group = me // pair
    member = lax.rem(me, pair)
    barrier = pltpu.get_barrier_semaphore()
    for step in range(1, groups):
        pl.semaphore_signal(
            barrier,
            inc=1,
            device_id={"sp": lax.rem(group + step, groups) * pair + member},
            device_id_type=MESH,
        )
    pl.semaphore_signal(
        barrier, inc=1, device_id={"sp": group * pair + 1 - member}, device_id_type=MESH
    )
    pl.semaphore_wait(barrier, groups)
    return group, member


def dispatch_kernel(rows_ref, out_ref, send_far, recv_far, send_near, recv_near):
    groups = rows_ref.shape[0]
    pair = out_ref.shape[0]
    group, member = greet_group(groups, pair)
    partner = group * pair + 1 - member
    far = []
    for step in range(1, groups):
        target = lax.rem(group + step, groups)
        copy = pltpu.make_async_remote_copy(
            src_ref=rows_ref.at[target],
            dst_ref=out_ref.at[member, group],
            send_sem=send_far.at[step],
            recv_sem=recv_far.at[step],
            device_id={"sp": target * pair + member},
            device_id_type=MESH,
        )
        copy.start()
        far.append(copy)
    near = []
    for step in range(groups):
        origin = lax.rem(group - step + groups, groups)
        if step > 0:
            far[step - 1].wait_recv()
        copy = pltpu.make_async_remote_copy(
            src_ref=rows_ref.at[group] if step == 0 else out_ref.at[member, origin],
            dst_ref=out_ref.at[member, origin],
            send_sem=send_near.at[step],
            recv_sem=recv_near.at[step],
            device_id={"sp": partner},
            device_id_type=MESH,
        )
        copy.start()
        near.append(copy)
        if step == 0:
            out_ref[member, group] = rows_ref[group]
    for copy in far:
        copy.wait_send()
    for copy in near:
        copy.wait()


def dispatch(rows, pair):
    groups = rows.shape[0]
    return pl.pallas_call(
        dispatch_kernel,
        out_shape=jax.ShapeDtypeStruct((pair,) + rows.shape, rows.dtype),
        in_specs=[VMEM_SPEC],
        out_specs=VMEM_SPEC,
        scratch_shapes=[pltpu.SemaphoreType.DMA((groups,))] * 4,
        compiler_params=pltpu.CompilerParams(collective_id=1, has_side_effects=True),
        name="row_dispatch",
    )(rows)


def collect_kernel(parts_ref, out_ref, landed, joined, send_near, recv_near, send_far, recv_far):
    pair, groups = parts_ref.shape[:2]
    group, member = greet_group(groups, pair)
    partner = group * pair + 1 - member
    order = list(range(1, groups)) + [0]
    near = {}
    for step in order:
        target = lax.rem(group + step, groups)
        near[step] = pltpu.make_async_remote_copy(
            src_ref=parts_ref.at[1 - member, target],
            dst_ref=landed.at[target],
            send_sem=send_near.at[step],
            recv_sem=recv_near.at[step],
            device_id={"sp": partner},
            device_id_type=MESH,
        )
        near[step].start()
    far = []
    for step in order:
        target = lax.rem(group + step, groups)
        near[step].wait_recv()
        total = (
            parts_ref[member, target].astype(jnp.float32) + landed[target].astype(jnp.float32)
        ).astype(out_ref.dtype)
        if step == 0:
            out_ref[group] = total
        else:
            joined[target] = total
            copy = pltpu.make_async_remote_copy(
                src_ref=joined.at[target],
                dst_ref=out_ref.at[group],
                send_sem=send_far.at[step],
                recv_sem=recv_far.at[step],
                device_id={"sp": target * pair + member},
                device_id_type=MESH,
            )
            copy.start()
            far.append(copy)
    for step in order:
        near[step].wait_send()
    for copy in far:
        copy.wait()


def collect(parts):
    pair, groups = parts.shape[:2]
    return pl.pallas_call(
        collect_kernel,
        out_shape=jax.ShapeDtypeStruct(parts.shape[1:], parts.dtype),
        in_specs=[VMEM_SPEC],
        out_specs=VMEM_SPEC,
        scratch_shapes=[pltpu.VMEM(parts.shape[1:], parts.dtype)] * 2
        + [pltpu.SemaphoreType.DMA((groups,))] * 4,
        compiler_params=pltpu.CompilerParams(collective_id=2, has_side_effects=True),
        name="row_collect",
    )(parts)


def contract_kernel(share_ref, *refs):
    out_ref = refs[-1]
    stacks = [ref for ref in refs[:-1] if len(ref.shape) == 3]
    hidden = [ref for ref in refs[:-1] if len(ref.shape) == 2]
    total = None
    for part, (stack, index) in enumerate(
        (stack, index) for stack in stacks for index in range(stack.shape[0])
    ):
        term = jnp.dot(hidden[part][...], stack[index], preferred_element_type=jnp.float32)
        total = term if total is None else total + term
    out_ref[...] = (total * share_ref[...]).astype(out_ref.dtype)


def contract(hidden, stacks, shares):
    rows, depth = hidden[0].shape
    width = stacks[0].shape[2]
    tile = min(512, width)
    return pl.pallas_call(
        contract_kernel,
        out_shape=jax.ShapeDtypeStruct((rows, width), jnp.bfloat16),
        grid=(width // tile,),
        in_specs=[pl.BlockSpec((rows, 1), lambda i: (0, 0))]
        + [pl.BlockSpec((rows, depth), lambda i: (0, 0))] * len(hidden)
        + [pl.BlockSpec((stack.shape[0], depth, tile), lambda i: (0, 0, i)) for stack in stacks],
        out_specs=pl.BlockSpec((rows, tile), lambda i: (0, i)),
        compiler_params=pltpu.CompilerParams(vmem_limit_bytes=48 * 1024 * 1024),
        cost_estimate=pl.CostEstimate(
            flops=2 * rows * depth * width * len(hidden),
            bytes_accessed=2 * len(hidden) * depth * (rows + width) + 2 * rows * width,
            transcendentals=0,
        ),
        name="expert_contract",
    )(shares, *hidden, *stacks)


def spread_weights(weights):
    count = lax.axis_size("tp")
    if count != 4:
        gathered = [lax.all_gather(weight, "tp") for weight in weights]
        return [[weight] for weight in gathered]
    across = [[0, 2], [1, 3]]
    beside = [(t, t + 1 - 2 * (t % 2)) for t in range(count)]
    far = [lax.all_gather(weight, "tp", axis_index_groups=across) for weight in weights]
    relayed = [lax.ppermute(both, "tp", beside) for both in far]
    return [list(both) for both in zip(far, relayed)]


def rotate(payload_tensor, positions):
    channel_dimension = payload_tensor.shape[-1]
    half = channel_dimension // 2
    freq = rope_base ** (-jnp.arange(half, dtype=jnp.float32) * 2.0 / channel_dimension)
    angle = positions.astype(jnp.float32)[:, None, None] * freq[None, None, :]
    cosine = jnp.cos(angle)
    sine = jnp.sin(angle)
    first = payload_tensor[..., :half]
    second = payload_tensor[..., half:]
    return jnp.concatenate([first * cosine - second * sine, first * sine + second * cosine], -1)


def segment_terms(probe_tensor, lookup_tensor, payload_tensor, surge_forgetting, forgetting_speed):
    length = probe_tensor.shape[0]
    segment_tally = jnp.arange(length, dtype=jnp.float32)
    memory_matrix = (
        forgetting_speed[None, :] * segment_tally[:, None] + jnp.cumsum(surge_forgetting)[:, None]
    )
    causal = (segment_tally[:, None] >= segment_tally[None, :])[None]
    level_t = jnp.transpose(memory_matrix)
    gap = level_t[:, :, None] - level_t[:, None, :]
    decay = jnp.where(causal, jnp.exp(jnp.where(causal, gap, 0.0)), 0.0)
    attention_scores = jnp.einsum(
        "szr,yzr->zsy", probe_tensor, lookup_tensor, preferred_element_type=jnp.float32
    )
    weights = (attention_scores * decay).astype(jnp.bfloat16)
    inner = jnp.einsum("htm,mhe->the", weights, payload_tensor, preferred_element_type=jnp.float32)
    factor = jnp.exp(memory_matrix + forgetting_speed[None, :])
    tail = jnp.exp(memory_matrix[-1:, :] - memory_matrix)
    weighted_output = (lookup_tensor.astype(jnp.float32) * tail[:, :, None]).astype(jnp.bfloat16)
    state_update = jnp.einsum(
        "oup,our->upr", weighted_output, payload_tensor, preferred_element_type=jnp.float32
    )
    total = memory_matrix[-1] + forgetting_speed
    return (inner, factor, state_update, total)


def read_state(probe_tensor, state):
    return jnp.einsum(
        "thd,hde->the", probe_tensor.astype(jnp.float32), state, precision=lax.Precision.HIGHEST
    )


def keeping_multiplier(
    probe_source,
    lookup_tensor,
    payload_tensor,
    forgetting_speed,
    surge_forgetting,
    channel_dimension,
    segment_begin,
):
    length = probe_source.shape[0]
    heads = probe_source.shape[1] // channel_dimension
    places = segment_begin + jnp.arange(length, dtype=jnp.int32)
    spun_probe = rotate(
        probe_source.astype(jnp.float32).reshape(length, heads, channel_dimension), places
    ).astype(jnp.bfloat16)
    spun_lookup = (
        rotate(lookup_tensor.astype(jnp.float32).reshape(length, heads, channel_dimension), places)
        * channel_dimension ** (-0.5)
    ).astype(jnp.bfloat16)
    regrouped_payload = payload_tensor.reshape(length, heads, channel_dimension)
    block = min(512, length)
    count = length // block

    def divider_mark(array):
        return array.reshape((count, block) + array.shape[1:])

    state, level, local, reach = None, None, [], []
    for piece in zip(
        divider_mark(spun_probe),
        divider_mark(spun_lookup),
        divider_mark(regrouped_payload),
        divider_mark(surge_forgetting),
    ):
        inner, factor, state_update, total = segment_terms(*piece, forgetting_speed)
        if state is None:
            state, level = state_update, total
        else:
            inner = inner + factor[:, :, None] * read_state(piece[0], state)
            factor = factor * jnp.exp(level)[None, :]
            state, level = jnp.exp(total)[:, None, None] * state + state_update, level + total
        local.append(inner)
        reach.append(factor)
    return (
        spun_probe,
        jnp.concatenate(local, 0),
        jnp.concatenate(reach, 0),
        level,
        state,
    )


def finish(sublayer_final, emission_valve, scaling_coefficients):
    length, heads, channel_dimension = sublayer_final.shape
    normed = sublayer_final * lax.rsqrt(
        jnp.mean(sublayer_final * sublayer_final, -1, keepdims=True) + epsilon
    )
    gated = (
        normed.reshape(length, heads * channel_dimension)
        * scaling_coefficients[None, :]
        * jax.nn.silu(emission_valve.astype(jnp.float32))
    )
    return gated.astype(jnp.bfloat16)


def carried(states, levels):
    place = lax.axis_index("sp")
    count = states.shape[0]
    index = jnp.arange(count, dtype=jnp.int32)
    between = (index[None, :] > index[:, None]) & (index[None, :] < place)
    reach = jnp.sum(jnp.where(between[:, :, None], levels[None, :, :], 0.0), 1)
    weight = jnp.where((index < place)[:, None], jnp.exp(reach), 0.0)
    return jnp.sum(weight[:, :, None, None] * states.astype(jnp.float32), 0)


def slot_positions(chosen, experts, cap):
    listed = chosen.reshape(-1)
    matches = (listed[:, None] == jnp.arange(experts, dtype=jnp.int32)[None, :]).astype(jnp.int32)
    before = jnp.cumsum(matches, 0) - matches
    order = jnp.sum(before * matches, 1)
    return (listed * cap + order).reshape(chosen.shape)


def fill_slots(rows_in, chosen, experts, cap):
    count = rows_in.shape[0]
    places = slot_positions(chosen, experts, cap).reshape(-1)
    owners = jnp.repeat(jnp.arange(count, dtype=jnp.int32), 2)
    source = jnp.full((experts * cap,), count, jnp.int32).at[places].set(owners)
    padded = jnp.concatenate([rows_in, jnp.zeros((1, rows_in.shape[1]), rows_in.dtype)], 0)
    return padded[source].reshape(experts, cap, rows_in.shape[1])


def on_device(
    broad_probe_tensor,
    broad_lookup_tensor,
    broad_payload_tensor,
    broad_emission_valve,
    slim_probe_tensor,
    slim_lookup_tensor,
    slim_payload_tensor,
    slim_emission_valve,
    broad_forgetting_speed,
    slim_forgetting_speed,
    broad_channel_scaling,
    slim_channel_scaling,
    surge_forgetting,
    broad_emission_proj,
    slim_emission_proj,
    skip_stream,
    premix_scaling_coeffs,
    routed_specialist_ids,
    routed_specialist_shares,
    specialist_valve_proj,
    specialist_expand_proj,
    specialist_contract_proj,
):
    length = broad_probe_tensor.shape[0]
    segment_begin = lax.axis_index("sp") * length
    valve_all, expand_all, contract_all = spread_weights(
        [specialist_valve_proj[0], specialist_expand_proj[0], specialist_contract_proj[0]]
    )
    wide_result = keeping_multiplier(
        broad_probe_tensor,
        broad_lookup_tensor,
        broad_payload_tensor,
        broad_forgetting_speed,
        surge_forgetting,
        BROAD_CHANNEL_DIM,
        segment_begin,
    )
    narrow_result = keeping_multiplier(
        slim_probe_tensor,
        slim_lookup_tensor,
        slim_payload_tensor,
        slim_forgetting_speed,
        surge_forgetting,
        THIN_CHANNEL_DIM,
        segment_begin,
    )
    rows = skip_stream.shape[0]
    width = skip_stream.shape[1]
    experts = lax.axis_size("sp") * specialist_valve_proj.shape[0]
    cap = rows * GROUPS // experts
    pair = experts // GROUPS
    own_ids = lax.dynamic_slice_in_dim(routed_specialist_ids, lax.axis_index("tp") * rows, rows, 0)
    own_weights = lax.dynamic_slice_in_dim(
        routed_specialist_shares, lax.axis_index("tp") * rows, rows, 0
    )
    levels = jnp.concatenate([wide_result[3], narrow_result[3]])
    tile = levels
    if pair == 2:
        group_of = own_ids[:, 0] // pair
        named = group_of[:, None] == jnp.arange(GROUPS, dtype=jnp.int32)[None, :]
        rank = jnp.cumsum(named.astype(jnp.int32), 0) - 1
        own_slot = group_of * cap + jnp.sum(jnp.where(named, rank, 0), 1)
        holds = own_slot[None, :] == jnp.arange(GROUPS * cap, dtype=jnp.int32)[:, None]
        member_ids = own_ids - group_of[:, None] * pair
        slot_shares = []
        for member in range(pair):
            share = jnp.sum(jnp.where(member_ids == member, own_weights, 0.0), 1)
            slot_shares.append(jnp.sum(jnp.where(holds, share[None, :], 0.0), 1))
        tile = jnp.concatenate([levels] + slot_shares)
    tile_size = -(-tile.shape[0] // 1024) * 1024
    tile = jnp.pad(tile, (0, tile_size - tile.shape[0])).reshape(-1, 128)
    packed = jnp.concatenate(
        [wide_result[4].reshape(-1, 128), narrow_result[4].reshape(-1, 128)], 0
    ).astype(jnp.bfloat16)
    states, tiles = exchange(packed, tile)
    count = states.shape[0]
    tiles = tiles.reshape(count, -1)
    wide_heads = wide_result[3].shape[0]
    both_heads = levels.shape[0]
    cut = wide_result[4].size // 128
    incoming_wide = carried(
        states[:, :cut].reshape((count,) + wide_result[4].shape), tiles[:, :wide_heads]
    )
    incoming_narrow = carried(
        states[:, cut:].reshape((count,) + narrow_result[4].shape),
        tiles[:, wide_heads:both_heads],
    )
    mixed_wide = finish(
        wide_result[1] + wide_result[2][:, :, None] * read_state(wide_result[0], incoming_wide),
        broad_emission_valve,
        broad_channel_scaling,
    )
    mixed_narrow = finish(
        narrow_result[1] + narrow_result[2][:, :, None] * read_state(narrow_result[0], incoming_narrow),
        slim_emission_valve,
        slim_channel_scaling,
    )
    rows_wide, rows_narrow = (
        lax.all_to_all(mixed_wide, "tp", split_axis=0, concat_axis=1, tiled=True),
        lax.all_to_all(mixed_narrow, "tp", split_axis=0, concat_axis=1, tiled=True),
    )
    projected = jnp.dot(rows_wide, broad_emission_proj, preferred_element_type=jnp.float32)
    projected = projected + jnp.dot(
        rows_narrow, slim_emission_proj, preferred_element_type=jnp.float32
    )
    updated = skip_stream.astype(jnp.float32) + projected
    scale = lax.rsqrt(jnp.mean(updated * updated, -1, keepdims=True) + epsilon)
    normed = (updated * scale * premix_scaling_coeffs[None, :]).astype(jnp.bfloat16)
    if pair == 2:
        spread = holds.astype(jnp.bfloat16)
        filled = jnp.dot(spread, normed, preferred_element_type=jnp.float32).astype(jnp.bfloat16)
        slots = dispatch(filled.reshape(GROUPS, cap, width), pair).reshape(-1, width)
    else:
        own_places = slot_positions(own_ids, experts, cap)
        slots = lax.all_to_all(
            fill_slots(normed, own_ids, experts, cap), "sp", split_axis=0, concat_axis=0, tiled=True
        ).reshape(-1, width)
    hidden = []
    for valve_stack, expand_stack in zip(valve_all, expand_all):
        for part in range(valve_stack.shape[0]):
            emission_valve = jnp.dot(slots, valve_stack[part], preferred_element_type=jnp.float32)
            up = jnp.dot(slots, expand_stack[part], preferred_element_type=jnp.float32)
            hidden.append((jax.nn.silu(emission_valve) * up).astype(jnp.bfloat16))
    shares = jnp.ones((slots.shape[0], 1), jnp.float32)
    if pair == 2:
        place = lax.axis_index("sp")
        shares = tiles[:, both_heads : both_heads + pair * GROUPS * cap]
        shares = shares.reshape(GROUPS, pair, pair, GROUPS, cap)
        shares = lax.dynamic_index_in_dim(shares, place % pair, 2, False)
        shares = lax.dynamic_index_in_dim(shares, place // pair, 2, False)
        shares = jnp.transpose(shares, (1, 0, 2)).reshape(-1, 1)
    parts = contract(hidden, contract_all, shares)
    if pair == 2:
        returned = collect(parts.reshape(pair, GROUPS, cap, width)).reshape(-1, width)
        mixture = lax.dot_general(
            spread, returned, (((0,), (0,)), ((), ())), preferred_element_type=jnp.float32
        )
    else:
        returned = lax.all_to_all(
            parts.reshape(experts, cap, width),
            "sp",
            split_axis=0,
            concat_axis=0,
            tiled=True,
        )
        picked = returned.reshape(experts * cap, width)[own_places]
        mixture = jnp.sum(own_weights[:, :, None] * picked.astype(jnp.float32), 1)
    return (updated + mixture).astype(jnp.bfloat16)


def solution(mesh):
    return jax.shard_map(
        on_device,
        mesh=mesh,
        in_specs=(
            P("sp", "tp"),
            P("sp", "tp"),
            P("sp", "tp"),
            P("sp", "tp"),
            P("sp", "tp"),
            P("sp", "tp"),
            P("sp", "tp"),
            P("sp", "tp"),
            P("tp"),
            P("tp"),
            P("tp"),
            P("tp"),
            P("sp"),
            P(),
            P(),
            P(("sp", "tp"), None),
            P(),
            P("sp", None),
            P("sp", None),
            P("sp", None, "tp"),
            P("sp", None, "tp"),
            P("sp", "tp", None),
        ),
        out_specs=P(("sp", "tp"), None),
        check_vma=False,
    )
```
